256 devices in a mesh: dp: 4 (over x), kv: 32 (over z, y), tp: 2 (over core).
Axes of the slice: x: 4, y: 4, z: 8, core: 2. Of those that a mesh axis runs over, the one named last changes fastest.
Arguments:
- tokens: bfloat16 [64, 16, 4096], P('dp', None, 'kv'), may hold values from -64 to 64
- in_gain: bfloat16 [4096], P('kv'), may hold values from 0.099609375 to 1.8984375
- query_weight: bfloat16 [4096, 4096], P('kv', 'tp'), may hold values from -0.125 to 0.125
- key_weight: bfloat16 [4096, 4096], P('kv', 'tp'), may hold values from -0.125 to 0.125
- value_weight: bfloat16 [4096, 4096], P('kv', 'tp'), may hold values from -0.09375 to 0.09375
- out_weight: bfloat16 [4096, 4096], P('tp', 'kv'), may hold values from -0.1875 to 0.1875
- lambdas: float32 [16], P('tp'), may hold values from 0.3 to 0.8
- sub_gain: bfloat16 [256], replicated, may hold values from 0.099609375 to 1.8984375
- key_cache: bfloat16 [64, 1024, 16, 2, 128], P('dp', 'kv', 'tp'), may hold values from -248 to 248
- value_cache: bfloat16 [64, 1024, 16, 256], P('dp', 'kv', 'tp'), may hold values from -6 to 6
- cache_len: int32 [64], P('dp'), may hold values from 512 to 992
- accepted: int32 [64], P('dp'), may hold values from 0 to 16
- parents: int32 [64, 16], P('dp'), may hold values from -1 to 14, as said below
Outputs:
- output: bfloat16 [64, 16, 4096], P('dp', None, ('kv', 'tp'))
- key_cache_out: bfloat16 [64, 1024, 16, 2, 128], P('dp', 'kv', 'tp')
- value_cache_out: bfloat16 [64, 1024, 16, 256], P('dp', 'kv', 'tp')
The draws below stay inside these ranges and needn't reach their ends.
Inputs may be any that keep to these rules, and one draw needn't show every extreme that they name: `parents`: each proposal's parent is -1 (the text already in the cache) or one of the three proposals just before it; the last proposal's parent is the one just before it. Positions below cache_len plus accepted hold a sequence's text; the later ones are stale.
All inputs are finite; a program needn't handle non-finite values.
Results may differ from the reference program's by a relative error of at most 0.019.
The reference program's roundings to bfloat16 on the way count: a program that leaves them out, or rounds other values in their place, can miss the bound.
Values may be sent and summed in bfloat16 or wider, within the bound.
No kernel may reach another device: no remote copies, remote signals or barrier semaphores. Data moves between devices by JAX's collectives and lax.ppermute only.
A program may use at most 64 MiB of HBM per device.

```python
import math
import jax
import jax.numpy as jnp
from jax import lax

D = 4096
HD = 128
H = 16
P_SIZE = 16
POS_DEV = 32
BATCH = 64
LEN = 1024
N_TP = 2


def draw_tokens(key, part):
    key_one = jax.random.fold_in(key, 0)
    column = 10.0 ** (jnp.arange(D, dtype=jnp.float32) / D)
    values = jax.random.normal(key_one, (BATCH, P_SIZE, D), jnp.float32) * column
    return jnp.clip(values, -64.0, 64.0).astype(jnp.bfloat16)


def draw_key_cache(key, part):
    key_one = jax.random.fold_in(key, 0)
    noise = jnp.clip(jax.random.normal(key_one, (BATCH, LEN, H, 2, HD), jnp.float32) * 1.3, -8.0, 8.0)
    return noise.astype(jnp.bfloat16)


def draw_parents(key, part):
    step_back = jax.random.randint(key, (BATCH, P_SIZE), 0, 3)
    last_column = (jnp.arange(P_SIZE, dtype=jnp.int32) == P_SIZE - 1)[None, :]
    step_back = jnp.where(last_column, 0, step_back)
    return jnp.maximum(jnp.arange(P_SIZE, dtype=jnp.int32)[None, :] - 1 - step_back, -1).astype(jnp.int32)


def place_ends(result, own_key, least, largest):
    longest = result.shape.index(max(result.shape))
    spots = []
    for shift in (0, 1):
        where = [jax.random.randint(jax.random.fold_in(own_key, axis), (), 0, length) for axis, length in enumerate(result.shape)]
        where[longest] = (where[longest] + shift) % result.shape[longest]
        spots.append(tuple(where))
    return result.at[spots[0]].set(least).at[spots[1]].set(largest)


def levels(stream_key, extent, shards, smallest, high):
    def one(position, blocks):
        draws = jax.random.uniform(jax.random.fold_in(jax.random.fold_in(stream_key, 6), position), (blocks,), jnp.float32, smallest / len(shards), high / len(shards))
        return jnp.repeat(jnp.exp(draws), extent[position] // blocks).reshape((-1,) + (1,) * (len(extent) - position - 1))

    loudness = one(*shards[0])
    for cut in shards[1:]:
        loudness = loudness * one(*cut)
    return loudness


def gaussian(key, dims, deviation, most, pieces=(), kind=jnp.bfloat16):
    values = deviation * jax.random.normal(key, dims, jnp.float32)
    if pieces:
        values = values * levels(key, dims, pieces, -0.22, 0.18)
    return jnp.clip(values, -most, most).astype(kind)


def setup_inputs(seed: int = 0) -> dict:
    key_list = jax.random.split(jax.random.key(seed), 14)
    return {
        "tokens": draw_tokens(jax.random.fold_in(key_list[13], 71), 0),
        "in_gain": jnp.clip(1.0 + 0.18 * jax.random.normal(key_list[1], (D,), jnp.float32), 0.099609375, 1.8984375).astype(jnp.bfloat16),
        "query_weight": gaussian(key_list[2], (D, D), (D * 10 // 17) ** -0.5, 0.125, ((0, 32), (1, 2))),
        "key_weight": gaussian(key_list[3], (D, D), (D * 10 // 17) ** -0.5, 0.125, ((0, 32), (1, 2))),
        "value_weight": gaussian(key_list[4], (D, D), D ** -0.5, 0.09375, ((0, 32), (1, 2))),
        "out_weight": gaussian(key_list[5], (D, D), (D // 4) ** -0.5, 0.1875, ((0, 2), (1, 32))),
        "lambdas": jnp.clip(0.3 + 0.5 * jax.random.uniform(key_list[6], (H,), jnp.float32) ** levels(key_list[6], (H,), ((0, 2),), -0.2, 0.2), 0.3, 0.8),
        "sub_gain": jnp.clip(1.0 + 0.18 * jax.random.normal(key_list[7], (2 * HD,), jnp.float32), 0.099609375, 1.8984375).astype(jnp.bfloat16),
        "key_cache": draw_key_cache(jax.random.fold_in(key_list[13], 71), 0),
        "value_cache": gaussian(key_list[9], (BATCH, LEN, H, 2 * HD), 1.0, 6.0, ((0, 4), (1, 32), (2, 2))),
        "cache_len": place_ends(jax.random.randint(key_list[10], (BATCH,), LEN // 2, LEN - 2 * P_SIZE + 1), jax.random.fold_in(key_list[10], 1), LEN // 2, LEN - 2 * P_SIZE).astype(jnp.int32),
        "accepted": place_ends(jax.random.randint(key_list[11], (BATCH,), 0, P_SIZE + 1), jax.random.fold_in(key_list[11], 1), 0, P_SIZE).astype(jnp.int32),
        "parents": draw_parents(jax.random.fold_in(key_list[13], 71), 0),
    }


LAMBDA_SCALE = 0.2 + 0.6 * math.exp(-0.6)
NEG_FILL = -1e+30

def visible_links(parents):
    number = parents.shape[-1]
    identity = jnp.eye(number, dtype=jnp.float32)
    parent_links = (parents[..., :, None] == jnp.arange(number, dtype=jnp.int32)[None, :]).astype(jnp.float32)

    def extend(repeat, reached):
        return jnp.maximum(identity, jnp.einsum('bij,bjk->bik', parent_links, reached, precision=lax.Precision.HIGHEST))
    reached = lax.fori_loop(0, number, extend, jnp.broadcast_to(identity, parent_links.shape))
    depths = (lax.optimization_barrier(jnp.sum(reached, axis=-1)) - 1.0).astype(jnp.int32)
    return (reached > 0.5, depths)

def rotate(values, positions):
    half_dim = values.shape[-1] // 2
    frequency = 10000.0 ** (-jnp.arange(half_dim, dtype=jnp.float32) / half_dim)
    angles = positions.astype(jnp.float32)[..., None] * frequency
    cosine = jnp.cos(angles)[..., None, None, :]
    sine_part = jnp.sin(angles)[..., None, None, :]
    lower_half = values[..., :half_dim]
    upper_half = values[..., half_dim:]
    return jnp.concatenate([lower_half * cosine - upper_half * sine_part, upper_half * cosine + lower_half * sine_part], axis=-1)

def reference(tokens, in_gain, query_weight, key_weight, value_weight, out_weight, lambdas, sub_gain, key_cache, value_cache, cache_len, accepted, parents):
    batch_size, prop_count, width_all = tokens.shape
    head_count = lambdas.shape[0]
    head_dim = key_cache.shape[-1]
    tokens_wide = tokens.astype(jnp.float32)
    squares = lax.optimization_barrier(jnp.sum(tokens_wide * tokens_wide, axis=-1))
    row_scale = lax.rsqrt(squares / width_all + 1e-06)[..., None]
    normed = (tokens_wide * in_gain.astype(jnp.float32)).astype(jnp.bfloat16).reshape(batch_size * prop_count, width_all)
    starts = cache_len + accepted
    visible, depths = visible_links(parents)
    positions = starts[:, None] + depths

    def project(weight):
        product = jnp.dot(normed, weight, preferred_element_type=jnp.float32)
        return product.reshape(batch_size, prop_count, -1) * row_scale
    vec_shape = (batch_size, prop_count, head_count, 2, head_dim)
    queries = rotate(project(query_weight).reshape(vec_shape), positions).astype(jnp.bfloat16)
    new_keys = rotate(project(key_weight).reshape(vec_shape), positions).astype(jnp.bfloat16)
    new_values = project(value_weight).reshape(batch_size, prop_count, head_count, 2 * head_dim).astype(jnp.bfloat16)
    slot_index = starts[:, None] + jnp.arange(prop_count, dtype=jnp.int32)[None, :]
    seq_index = jnp.broadcast_to(jnp.arange(batch_size, dtype=jnp.int32)[:, None], slot_index.shape)
    key_out = key_cache.at[seq_index, slot_index].set(new_keys)
    value_out = value_cache.at[seq_index, slot_index].set(new_values)
    lam_mix = lambdas[:, None, None]
    inverse_root = head_dim ** (-0.5)

    def one_sequence(sequence_items):
        query_rows, key_new, value_new, key_rows, value_rows, start_pos, seen_mask = sequence_items
        length = key_rows.shape[0]
        query_wide = query_rows.astype(jnp.float32)
        cache_scores = jnp.einsum('qhmd,thmd->hmqt', query_wide, key_rows.astype(jnp.float32)) * inverse_root
        live_mask = (jnp.arange(length, dtype=jnp.int32) < start_pos)[None, None, None, :]
        cache_scores = jnp.where(live_mask, cache_scores, NEG_FILL)
        own_scores = jnp.einsum('qhmd,jhmd->hmqj', query_wide, key_new.astype(jnp.float32)) * inverse_root
        own_mask = seen_mask[None, None]
        own_scores = jnp.where(own_mask, own_scores, NEG_FILL)
        highest = jnp.maximum(lax.optimization_barrier(jnp.max(cache_scores, axis=-1)), lax.optimization_barrier(jnp.max(own_scores, axis=-1)))
        cache_exp = jnp.where(live_mask, jnp.exp(cache_scores - highest[..., None]), 0.0)
        own_exp = jnp.where(own_mask, jnp.exp(own_scores - highest[..., None]), 0.0)
        totals = lax.optimization_barrier(jnp.sum(cache_exp, axis=-1)) + lax.optimization_barrier(jnp.sum(own_exp, axis=-1))
        cache_prob = cache_exp / totals[..., None]
        own_prob = own_exp / totals[..., None]
        cache_weight = (cache_prob[:, 0] - lam_mix * cache_prob[:, 1]).astype(jnp.bfloat16)
        own_weight = (own_prob[:, 0] - lam_mix * own_prob[:, 1]).astype(jnp.bfloat16)
        blocks = length // POS_DEV
        block_weight = cache_weight.reshape(head_count, prop_count, blocks, POS_DEV).astype(jnp.float32)
        block_values = value_rows.reshape(blocks, POS_DEV, head_count, 2 * head_dim).astype(jnp.float32)
        partial_value = jnp.einsum('hqnt,nthe->nqhe', block_weight, block_values)
        partial_value = lax.optimization_barrier(partial_value.astype(jnp.bfloat16)).astype(jnp.float32)
        own_term = jnp.einsum('hqj,jhe->qhe', own_weight.astype(jnp.float32), value_new.astype(jnp.float32))
        return lax.optimization_barrier(jnp.sum(partial_value, axis=0)) + own_term
    attended = lax.map(one_sequence, (queries, new_keys, new_values, key_cache, value_cache, starts, visible))
    mixed_out = attended * lax.rsqrt(lax.optimization_barrier(jnp.mean(attended * attended, axis=-1, keepdims=True)) + 1e-05)
    mixed_out = (mixed_out * sub_gain.astype(jnp.float32) * LAMBDA_SCALE).astype(jnp.bfloat16)
    mixed_out = mixed_out.reshape(batch_size * prop_count, head_count * 2 * head_dim)
    group_cols = head_count * 2 * head_dim // N_TP
    totals_out = jnp.zeros((batch_size * prop_count, width_all), jnp.float32)
    for member in range(N_TP):
        product = jnp.dot(mixed_out[:, member * group_cols:(member + 1) * group_cols], out_weight[member * group_cols:(member + 1) * group_cols], preferred_element_type=jnp.float32)
        totals_out = totals_out + lax.optimization_barrier(product.astype(jnp.bfloat16)).astype(jnp.float32)
    output = totals_out.astype(jnp.bfloat16).reshape(batch_size, prop_count, width_all)
    return (output, key_out, value_out)
```

```python
import math

import jax
import jax.numpy as jnp
from jax import lax
from jax.experimental import pallas as pl
from jax.experimental.pallas import tpu as pltpu
from jax.sharding import Mesh
from jax.sharding import PartitionSpec as P

D = 4096
KV = ("kv_0", "kv_1")
KV_TP = ("kv_0", "kv_1", "tp")
LAMBDA_SCALE = 0.2 + 0.6 * math.exp(-0.6)
NEG_FILL = -1e30

GROUPS = 4
HEADS = 8
SEQS = 4
PROPS = 16
ROWS = SEQS * PROPS
SPAN = 32
HD = 128
STAT_ROWS = 8
O_ROWS = SEQS * 2 * PROPS
O_STATS = 16


def three_terms(x):
    high = x.astype(jnp.bfloat16)
    rest = x - high.astype(jnp.float32)
    middle = rest.astype(jnp.bfloat16)
    low = (rest - middle.astype(jnp.float32)).astype(jnp.bfloat16)
    return high, middle, low


def project_kernel(tokens_ref, gain_ref, wq_ref, wk_ref, wv_ref, out_ref):
    tokens = tokens_ref[...].astype(jnp.float32)
    normed = (tokens * gain_ref[...].astype(jnp.float32)).astype(jnp.bfloat16)
    for part, ref in enumerate((wq_ref, wk_ref, wv_ref)):
        product = jnp.dot(normed, ref[...], preferred_element_type=jnp.float32)
        product = product.astype(jnp.bfloat16)
        for g in range(GROUPS):
            out_ref[g, 0, 0:ROWS, part * 256 : (part + 1) * 256] = product[
                g * ROWS : (g + 1) * ROWS
            ]
    square = tokens * tokens
    high, low, _ = three_terms(square)
    ones = jnp.ones((8, tokens.shape[1]), jnp.bfloat16)
    contract = (((1,), (1,)), ((), ()))
    power = lax.dot_general(ones, high, contract, preferred_element_type=jnp.float32)
    power = power + lax.dot_general(ones, low, contract, preferred_element_type=jnp.float32)
    terms = [t.astype(jnp.float32) for t in three_terms(power)]
    row = lax.broadcasted_iota(jnp.int32, power.shape, 0)
    zero = jnp.zeros_like(power)
    stats = jnp.where(row == 0, terms[0], zero)
    stats = jnp.where(row == 1, terms[1], stats)
    stats = jnp.where(row == 2, terms[2], stats)
    stats = stats.astype(jnp.bfloat16)
    blank = jnp.zeros((STAT_ROWS, 256), jnp.bfloat16)
    for g in range(GROUPS):
        out_ref[g, 0, ROWS : ROWS + STAT_ROWS, 0:256] = stats
        out_ref[g, 0, ROWS : ROWS + STAT_ROWS, 256:512] = blank
        out_ref[g, 0, ROWS : ROWS + STAT_ROWS, 512:768] = blank


def partial_products(tokens, gain, wq, wk, wv):
    rows, width = tokens.shape
    weight_spec = pl.BlockSpec((width, 256), lambda h: (0, h))
    return pl.pallas_call(
        project_kernel,
        grid=(HEADS,),
        in_specs=[
            pl.BlockSpec((rows, width), lambda h: (0, 0)),
            pl.BlockSpec((1, width), lambda h: (0, 0)),
            weight_spec,
            weight_spec,
            weight_spec,
        ],
        out_specs=pl.BlockSpec((GROUPS, 1, ROWS + STAT_ROWS, 768), lambda h: (0, h, 0, 0)),
        out_shape=jax.ShapeDtypeStruct((GROUPS, HEADS, ROWS + STAT_ROWS, 768), jnp.bfloat16),
        name="partial_products",
    )(tokens, gain, wq, wk, wv)


def attend_kernel(starts_ref, offset_ref, got_ref, k_ref, v_ref, o_ref, ko_ref, vo_ref):
    group = pl.program_id(0)
    offset = offset_ref[0]
    key_rows = SPAN * HEADS * 2
    cols = HEADS * 2 * PROPS
    row = lax.broadcasted_iota(jnp.int32, (key_rows, cols), 0)
    col = lax.broadcasted_iota(jnp.int32, (key_rows, cols), 1)
    same = (row % 16) == (col // PROPS)
    pair_row = lax.broadcasted_iota(jnp.int32, (SPAN * HEADS, key_rows), 0)
    pair_col = lax.broadcasted_iota(jnp.int32, (SPAN * HEADS, key_rows), 1)
    pairs = jnp.where(pair_row == pair_col // 2, 1.0, 0.0).astype(jnp.bfloat16)
    stats = []
    for s in range(SEQS):
        start = starts_ref[group * SEQS + s]
        first = start - offset
        lines = slice(s * PROPS, (s + 1) * PROPS)
        query = jnp.stack(
            [got_ref[0, :, lines, 0:HD], got_ref[0, :, lines, HD : 2 * HD]], axis=1
        ).reshape(cols, HD)
        keys = k_ref[s]
        values = v_ref[s]
        scores = lax.dot_general(
            keys, query, (((1,), (1,)), ((), ())), preferred_element_type=jnp.float32
        ) * (HD**-0.5)
        alive = same & (row < 16 * first)
        scores = jnp.where(alive, scores, NEG_FILL)
        peak = jnp.max(scores, axis=0, keepdims=True)
        weight = jnp.where(alive, jnp.exp(scores - peak), 0.0)
        total = jnp.sum(weight, axis=0, keepdims=True)
        some = total > 0.0
        safe = jnp.where(some, total, 1.0)
        weight = (weight * (1.0 / safe)).astype(jnp.bfloat16)
        level = jnp.where(some, peak + jnp.log(safe), NEG_FILL)
        stats.extend(t.astype(jnp.float32) for t in three_terms(level))
        weight = jnp.dot(pairs, weight, preferred_element_type=jnp.float32).astype(jnp.bfloat16)
        summed = lax.dot_general(
            weight, values, (((0,), (0,)), ((), ())), preferred_element_type=jnp.float32
        ).astype(jnp.bfloat16)
        for h in range(HEADS):
            o_ref[0, h, s * 32 : (s + 1) * 32, :] = summed[h * 32 : (h + 1) * 32]
        ko_ref[s] = keys
        vo_ref[s] = values

        @pl.when((first > -PROPS) & (first < SPAN))
        def _():
            lane = lax.broadcasted_iota(jnp.int32, (SPAN * HEADS, HEADS * PROPS), 1)
            line = lax.broadcasted_iota(jnp.int32, (SPAN * HEADS, HEADS * PROPS), 0)
            pick = ((line % HEADS) == (lane // PROPS)) & ((line // HEADS - first) == lane % PROPS)
            pick = jnp.where(pick, 1.0, 0.0).astype(jnp.bfloat16)
            fresh = jnp.dot(
                pick,
                got_ref[0, :, lines, 512:768].reshape(HEADS * PROPS, 256),
                preferred_element_type=jnp.float32,
            )
            at = lax.broadcasted_iota(jnp.int32, fresh.shape, 0) // HEADS - first
            inside = (at >= 0) & (at < PROPS)
            vo_ref[s] = jnp.where(inside, fresh, values.astype(jnp.float32)).astype(jnp.bfloat16)
            lane = lax.broadcasted_iota(jnp.int32, (key_rows, HEADS * PROPS), 1)
            line = lax.broadcasted_iota(jnp.int32, (key_rows, HEADS * PROPS), 0)
            here = (((line // 2) % HEADS) == (lane // PROPS)) & (
                (line // 16 - first) == lane % PROPS
            )
            fresh = jnp.zeros((key_rows, HD), jnp.float32)
            for m in range(2):
                pick = jnp.where(here & (line % 2 == m), 1.0, 0.0).astype(jnp.bfloat16)
                rows_new = got_ref[0, :, lines, 256 + m * HD : 256 + (m + 1) * HD]
                fresh = fresh + jnp.dot(
                    pick, rows_new.reshape(HEADS * PROPS, HD), preferred_element_type=jnp.float32
                )
            at = lax.broadcasted_iota(jnp.int32, fresh.shape, 0) // 16 - first
            inside = (at >= 0) & (at < PROPS)
            ko_ref[s] = jnp.where(inside, fresh, keys.astype(jnp.float32)).astype(jnp.bfloat16)

    stats.append(jnp.zeros((O_STATS - len(stats), cols), jnp.float32))
    stats = jnp.concatenate(stats, axis=0).astype(jnp.bfloat16)
    for h in range(HEADS):
        o_ref[0, h, O_ROWS : O_ROWS + O_STATS, :] = stats


def attend(starts, offset, got, keys, values):
    smem = pl.BlockSpec(memory_space=pltpu.SMEM)
    key_rows = SPAN * HEADS * 2
    return pl.pallas_call(
        attend_kernel,
        grid=(GROUPS,),
        in_specs=[
            smem,
            smem,
            pl.BlockSpec((1, HEADS, ROWS, 768), lambda g: (g, 0, 0, 0)),
            pl.BlockSpec((SEQS, key_rows, HD), lambda g: (g, 0, 0)),
            pl.BlockSpec((SEQS, SPAN * HEADS, 256), lambda g: (g, 0, 0)),
        ],
        out_specs=[
            pl.BlockSpec((1, HEADS, O_ROWS + O_STATS, 256), lambda g: (g, 0, 0, 0)),
            pl.BlockSpec((SEQS, key_rows, HD), lambda g: (g, 0, 0)),
            pl.BlockSpec((SEQS, SPAN * HEADS, 256), lambda g: (g, 0, 0)),
        ],
        out_shape=[
            jax.ShapeDtypeStruct((GROUPS, HEADS, O_ROWS + O_STATS, 256), jnp.bfloat16),
            jax.ShapeDtypeStruct(keys.shape, jnp.bfloat16),
            jax.ShapeDtypeStruct(values.shape, jnp.bfloat16),
        ],
        name="attend",
    )(starts, offset, got, keys, values)


def visible_links(parents):
    number = parents.shape[-1]
    reached = jnp.eye(number, dtype=jnp.float32) + (
        parents[..., :, None] == jnp.arange(number, dtype=jnp.int32)
    ).astype(jnp.float32)
    for _ in range(4):
        reached = jnp.minimum(jnp.einsum("bij,bjk->bik", reached, reached), 1.0)
    depths = (jnp.sum(reached, axis=-1) - 1.0).astype(jnp.int32)
    return reached > 0.5, depths


def to_all(value):
    size = lax.axis_size(KV)
    return lax.all_to_all(
        jnp.broadcast_to(value[None], (size, *value.shape)), KV, 0, 0, tiled=True
    )


def per_device(
    tokens,
    in_gain,
    query_weight,
    key_weight,
    value_weight,
    out_weight,
    lambdas,
    sub_gain,
    key_cache,
    value_cache,
    cache_len,
    accepted,
    parents,
):
    seq_count, prop_count, width_part = tokens.shape
    row_count = seq_count * prop_count
    me = lax.axis_index(KV)
    group = me // HEADS
    head = me % HEADS
    starts = cache_len + accepted
    partial = partial_products(
        tokens.reshape(row_count, width_part),
        in_gain.reshape(1, width_part),
        query_weight,
        key_weight,
        value_weight,
    )
    arrived = lax.all_to_all(
        partial.reshape(GROUPS * HEADS, ROWS + STAT_ROWS, 768), KV, 0, 0, tiled=True
    )
    summed = jnp.sum(arrived.astype(jnp.float32), axis=0)
    power = jnp.sum(summed[ROWS : ROWS + 3, 0:256], axis=0)
    power = lax.dynamic_slice(power, (group * ROWS,), (ROWS,))
    row_scale = lax.rsqrt(power / D + 1e-06)
    scaled = summed[:ROWS] * row_scale[:, None]
    own_starts = lax.dynamic_slice(starts, (group * SEQS,), (SEQS,))
    own_parents = lax.dynamic_slice(parents, (group * SEQS, 0), (SEQS, prop_count))
    visible, depths = visible_links(own_parents)
    positions = (own_starts[:, None] + depths).reshape(ROWS)
    half_dim = HD // 2
    frequency = 10000.0 ** (-jnp.arange(half_dim, dtype=jnp.float32) / half_dim)
    angles = positions.astype(jnp.float32)[:, None] * frequency[None, :]
    cosine = jnp.cos(angles)[:, None]
    sine = jnp.sin(angles)[:, None]
    vectors = scaled[:, :512].reshape(ROWS, 4, HD)
    lower = vectors[..., :half_dim]
    upper = vectors[..., half_dim:]
    turned = jnp.concatenate(
        [lower * cosine - upper * sine, upper * cosine + lower * sine], axis=-1
    ).reshape(ROWS, 512)
    own = jnp.concatenate([turned, scaled[:, 512:]], axis=1).astype(jnp.bfloat16)
    got = to_all(own).reshape(GROUPS, HEADS, ROWS, 768)
    offset = (me * SPAN).astype(jnp.int32).reshape(1)
    parts, key_out, value_out = attend(
        starts,
        offset,
        got,
        key_cache.reshape(seq_count, SPAN * HEADS * 2, HD),
        value_cache.reshape(seq_count, SPAN * HEADS, 256),
    )
    merged = lax.all_to_all(
        parts.reshape(GROUPS * HEADS, O_ROWS + O_STATS, 256), KV, 0, 0, tiled=True
    )
    levels = merged[:, O_ROWS : O_ROWS + 3 * SEQS].astype(jnp.float32)
    levels = lax.dynamic_slice(levels, (0, 0, head * 32), (32, 3 * SEQS, 32))
    levels = jnp.sum(levels.reshape(32, SEQS, 3, 32), axis=2).reshape(32, SEQS, 2, PROPS)
    own_blocks = own.reshape(SEQS, PROPS, 6, HD)
    own_scores = jnp.einsum(
        "sqmd,sjmd->smqj",
        own_blocks[:, :, 0:2],
        own_blocks[:, :, 2:4],
        preferred_element_type=jnp.float32,
    ) * (HD**-0.5)
    seen = visible[:, None]
    own_scores = jnp.where(seen, own_scores, NEG_FILL)
    peak = jnp.maximum(jnp.max(own_scores, axis=-1), jnp.max(levels, axis=0))
    own_weight = jnp.where(seen, jnp.exp(own_scores - peak[..., None]), 0.0)
    share = jnp.exp(levels - peak[None])
    total = jnp.sum(own_weight, axis=-1) + jnp.sum(share, axis=0)
    lam = lax.dynamic_slice(lambdas, (head,), (1,))
    sign = jnp.concatenate([jnp.ones((1,), jnp.float32), -lam])[None, :, None] / total
    share = share * sign[None]
    own_weight = own_weight * sign[..., None]
    own_mix = jnp.sum(own_weight, axis=1).astype(jnp.bfloat16)
    own_values = own[:, 512:].reshape(SEQS, PROPS, 256)
    attended = jnp.sum(
        merged[:, :O_ROWS].astype(jnp.float32).reshape(32, SEQS, 2, PROPS, 256)
        * share[..., None],
        axis=(0, 2),
    )
    attended = attended + jnp.einsum(
        "sqj,sje->sqe", own_mix, own_values, preferred_element_type=jnp.float32
    )
    mixed = attended * lax.rsqrt(jnp.mean(attended * attended, axis=-1, keepdims=True) + 1e-05)
    mixed = (mixed * sub_gain.astype(jnp.float32) * LAMBDA_SCALE).astype(jnp.bfloat16)
    mixed_all = to_all(mixed.reshape(ROWS, 256)).reshape(GROUPS, HEADS, ROWS, 256)
    product = jnp.einsum(
        "ghre,hec->grc",
        mixed_all,
        out_weight.reshape(HEADS, 256, -1),
        preferred_element_type=jnp.float32,
    ).astype(jnp.bfloat16)
    halves = jnp.moveaxis(product.reshape(row_count, 2, -1), 1, 0)
    both = lax.all_to_all(halves, "tp", 0, 0, tiled=True).astype(jnp.float32)
    output = (both[0] + both[1]).astype(jnp.bfloat16).reshape(seq_count, prop_count, -1)
    return (output, key_out.reshape(key_cache.shape), value_out.reshape(value_cache.shape))


def solution(mesh):
    torus = Mesh(
        mesh.devices.reshape(mesh.shape["dp"], 8, 4, mesh.shape["tp"]), ("dp", "kv_0", "kv_1", "tp")
    )
    placed = (
        P("dp", None, KV),
        P(KV),
        P(KV, "tp"),
        P(KV, "tp"),
        P(KV, "tp"),
        P("tp", KV),
        P("tp"),
        P(),
        P("dp", KV, "tp", None, None),
        P("dp", KV, "tp", None),
        P("dp"),
        P("dp"),
        P("dp", None),
    )
    return jax.shard_map(
        per_device,
        mesh=torus,
        in_specs=placed,
        out_specs=(P("dp", None, KV_TP), P("dp", KV, "tp", None, None), P("dp", KV, "tp", None)),
        check_vma=False,
    )
```

```python
import math

import jax
import jax.numpy as jnp
from jax import lax
from jax.experimental import pallas as pl
from jax.experimental.pallas import tpu as pltpu
from jax.sharding import Mesh
from jax.sharding import PartitionSpec as P

D = 4096
LAMBDA_SCALE = 0.2 + 0.6 * math.exp(-0.6)
NEG_FILL = -1e30

GROUPS = 4
HEADS = 8
SEQS = 4
PROPS = 16
ROWS = SEQS * PROPS
ALL_ROWS = GROUPS * ROWS
SPAN = 32
HD = 128
WIDTH = 128
EXTRA = 8
O_ROWS = SEQS * 2 * PROPS
O_STATS = 16
G = ("zl", "y")
KV = ("zh", "zl", "y")


def three_terms(x):
    high = x.astype(jnp.bfloat16)
    rest = x - high.astype(jnp.float32)
    middle = rest.astype(jnp.bfloat16)
    low = (rest - middle.astype(jnp.float32)).astype(jnp.bfloat16)
    return high, middle, low


def term_rows(x, count):
    terms = [t.astype(jnp.float32) for t in three_terms(x)]
    row = lax.broadcasted_iota(jnp.int32, (count, x.shape[1]), 0)
    result = jnp.zeros((count, x.shape[1]), jnp.float32)
    for k, term in enumerate(terms):
        result = jnp.where(row == k, term[0:1], result)
    return result.astype(jnp.bfloat16)


def pack_kernel(tokens_ref, gain_ref, wq_ref, wk_ref, wv_ref, out_ref, side_ref):
    @pl.when(pl.program_id(0) == 0)
    def _():
        tokens = tokens_ref[...].astype(jnp.float32)
        normed = (tokens * gain_ref[...].astype(jnp.float32)).astype(jnp.bfloat16)
        side_ref[0:WIDTH, :] = normed.astype(jnp.float32).T.astype(jnp.bfloat16)
        square = tokens * tokens
        high, low, _ = three_terms(square)
        ones = jnp.ones((8, WIDTH), jnp.bfloat16)
        contract = (((1,), (1,)), ((), ()))
        power = lax.dot_general(ones, high, contract, preferred_element_type=jnp.float32)
        power = power + lax.dot_general(ones, low, contract, preferred_element_type=jnp.float32)
        side_ref[WIDTH : WIDTH + EXTRA, :] = term_rows(power, EXTRA)

    for part, ref in enumerate((wq_ref, wk_ref, wv_ref)):
        out_ref[0, 0:WIDTH, part * 256 : (part + 1) * 256] = ref[...]
        out_ref[0, WIDTH : WIDTH + EXTRA, part * 256 : (part + 1) * 256] = jnp.zeros(
            (EXTRA, 256), jnp.bfloat16
        )
    out_ref[0, :, 768:1024] = side_ref[...]


def packed_pieces(tokens, gain, wq, wk, wv):
    rows, width = tokens.shape
    weight_spec = pl.BlockSpec((width, 256), lambda h: (0, h))
    return pl.pallas_call(
        pack_kernel,
        grid=(HEADS,),
        in_specs=[
            pl.BlockSpec((rows, width), lambda h: (0, 0)),
            pl.BlockSpec((1, width), lambda h: (0, 0)),
            weight_spec,
            weight_spec,
            weight_spec,
        ],
        out_specs=pl.BlockSpec((1, WIDTH + EXTRA, 1024), lambda h: (h, 0, 0)),
        out_shape=jax.ShapeDtypeStruct((HEADS, WIDTH + EXTRA, 1024), jnp.bfloat16),
        scratch_shapes=[pltpu.VMEM((WIDTH + EXTRA, ALL_ROWS), jnp.bfloat16)],
        name="packed_pieces",
    )(tokens, gain, wq, wk, wv)


def project_kernel(zh_ref, got_ref, *rest):
    outs, sum_ref, power_ref = rest[:GROUPS], rest[GROUPS], rest[GROUPS + 1]
    step = pl.program_id(0)
    product = lax.dot_general(
        got_ref[0, 0:WIDTH, 768:1024],
        got_ref[0, 0:WIDTH, 0:768],
        (((0,), (0,)), ((), ())),
        preferred_element_type=jnp.float32,
    )
    power = jnp.sum(
        got_ref[0, WIDTH : WIDTH + EXTRA, 768:1024].astype(jnp.float32), axis=0, keepdims=True
    )
    power = jnp.broadcast_to(power, power_ref.shape)

    @pl.when(step == 0)
    def _():
        sum_ref[...] = product
        power_ref[...] = power

    @pl.when(step > 0)
    def _():
        sum_ref[...] += product
        power_ref[...] += power

    @pl.when(step == HEADS - 1)
    def _():
        stats = term_rows(power_ref[...], EXTRA)
        for k, out in enumerate(outs):
            group = (zh_ref[0] + k) % GROUPS
            lines = pl.ds(pl.multiple_of(group * ROWS, ROWS), ROWS)
            out[0:ROWS, :] = sum_ref[lines, :].astype(jnp.bfloat16)
            out[ROWS : ROWS + EXTRA, 0:256] = stats
            out[ROWS : ROWS + EXTRA, 256:768] = jnp.zeros((EXTRA, 512), jnp.bfloat16)


def projected(zh, got):
    return pl.pallas_call(
        project_kernel,
        grid=(HEADS,),
        in_specs=[
            pl.BlockSpec(memory_space=pltpu.SMEM),
            pl.BlockSpec((1, WIDTH + EXTRA, 1024), lambda h: (h, 0, 0)),
        ],
        out_specs=[pl.BlockSpec((ROWS + EXTRA, 768), lambda h: (0, 0))] * GROUPS,
        out_shape=[jax.ShapeDtypeStruct((ROWS + EXTRA, 768), jnp.bfloat16)] * GROUPS,
        scratch_shapes=[
            pltpu.VMEM((ALL_ROWS, 768), jnp.float32),
            pltpu.VMEM((8, ALL_ROWS), jnp.float32),
        ],
        name="projected",
    )(zh, got)


def attend_kernel(starts_ref, offset_ref, got_ref, k_ref, v_ref, o_ref, pick_ref, stat_ref):
    group = pl.program_id(0)
    s = pl.program_id(1)
    pairs = SPAN * HEADS
    cols = HEADS * PROPS

    @pl.when((group == 0) & (s == 0))
    def _():
        line = lax.broadcasted_iota(jnp.int32, (pairs, 2 * pairs), 0)
        lane = lax.broadcasted_iota(jnp.int32, (pairs, 2 * pairs), 1)
        for m in range(2):
            pick_ref[m] = jnp.where(lane == 2 * line + m, 1.0, 0.0).astype(jnp.bfloat16)

    first = starts_ref[group * SEQS + s] - offset_ref[0]
    row = lax.broadcasted_iota(jnp.int32, (pairs, cols), 0)
    col = lax.broadcasted_iota(jnp.int32, (pairs, cols), 1)
    alive = ((row % HEADS) == (col // PROPS)) & (row < HEADS * first)
    lines = pl.ds(pl.multiple_of(s * PROPS, PROPS), PROPS)
    keys = k_ref[0]
    values = v_ref[0]
    for m in range(2):
        query = got_ref[0, :, lines, m * HD : (m + 1) * HD].reshape(cols, HD)
        keys_m = jnp.dot(pick_ref[m], keys, preferred_element_type=jnp.float32).astype(
            jnp.bfloat16
        )
        scores = lax.dot_general(
            keys_m, query, (((1,), (1,)), ((), ())), preferred_element_type=jnp.float32
        ) * (HD**-0.5)
        scores = jnp.where(alive, scores, NEG_FILL)
        peak = jnp.max(scores, axis=0, keepdims=True)
        weight = jnp.where(alive, jnp.exp(scores - peak), 0.0)
        total = jnp.sum(weight, axis=0, keepdims=True)
        some = total > 0.0
        safe = jnp.where(some, total, 1.0)
        weight = (weight * (1.0 / safe)).astype(jnp.bfloat16)
        level = jnp.where(some, peak + jnp.log(safe), NEG_FILL)
        stat_row = lax.broadcasted_iota(jnp.int32, (O_STATS, cols), 0)
        stats = stat_ref[:, m * cols : (m + 1) * cols]
        for k, term in enumerate(three_terms(level)):
            stats = jnp.where(stat_row == 3 * s + k, term.astype(jnp.float32), stats)
        stat_ref[:, m * cols : (m + 1) * cols] = stats
        summed = lax.dot_general(
            weight, values, (((0,), (0,)), ((), ())), preferred_element_type=jnp.float32
        ).astype(jnp.bfloat16)
        for h in range(HEADS):
            at = pl.multiple_of(s * 2 * PROPS + m * PROPS, PROPS)
            o_ref[h, 0, pl.ds(at, PROPS), :] = summed[h * PROPS : (h + 1) * PROPS]

    @pl.when(s == SEQS - 1)
    def _():
        row = lax.broadcasted_iota(jnp.int32, (O_STATS, 256), 0)
        stats = jnp.where(row < 3 * SEQS, stat_ref[...], 0.0).astype(jnp.bfloat16)
        for h in range(HEADS):
            o_ref[h, 0, O_ROWS : O_ROWS + O_STATS, :] = stats


def attend(starts, offset, got, keys, values):
    smem = pl.BlockSpec(memory_space=pltpu.SMEM)
    pairs = SPAN * HEADS
    return pl.pallas_call(
        attend_kernel,
        grid=(GROUPS, SEQS),
        in_specs=[
            smem,
            smem,
            pl.BlockSpec((1, HEADS, ROWS, 256), lambda g, s: (g, 0, 0, 0)),
            pl.BlockSpec((1, 2 * pairs, HD), lambda g, s: (g * SEQS + s, 0, 0)),
            pl.BlockSpec((1, pairs, 256), lambda g, s: (g * SEQS + s, 0, 0)),
        ],
        out_specs=pl.BlockSpec((HEADS, 1, O_ROWS + O_STATS, 256), lambda g, s: (0, g, 0, 0)),
        out_shape=jax.ShapeDtypeStruct((HEADS, GROUPS, O_ROWS + O_STATS, 256), jnp.bfloat16),
        scratch_shapes=[
            pltpu.VMEM((2, pairs, 2 * pairs), jnp.bfloat16),
            pltpu.VMEM((O_STATS, 256), jnp.float32),
        ],
        cost_estimate=pl.CostEstimate(
            flops=2 * 10**9, transcendentals=2 * 10**6, bytes_accessed=8 * 2**20
        ),
        name="attend",
    )(starts, offset, got, keys, values)


def write_kernel(scalars_ref, k_ref, v_ref, *rest):
    new_refs, (ko_ref, vo_ref) = rest[:HEADS], rest[HEADS:]
    seq = pl.program_id(0)
    zl = scalars_ref[1]
    y = scalars_ref[2]
    first = scalars_ref[4 + seq] - scalars_ref[3]
    keys = k_ref[0]
    values = v_ref[0]
    ko_ref[0] = keys
    vo_ref[0] = values

    @pl.when((first > -PROPS) & (first < SPAN))
    def _():
        fresh_all = jnp.concatenate([ref[0] for ref in new_refs], axis=0)
        lane = lax.broadcasted_iota(jnp.int32, (SPAN * HEADS, HEADS * PROPS), 1)
        line = lax.broadcasted_iota(jnp.int32, (SPAN * HEADS, HEADS * PROPS), 0)
        slot = lane // PROPS
        head = ((slot // 4 + zl) % 2) * 4 + (slot % 4 + y) % 4
        pick = ((line % HEADS) == head) & ((line // HEADS - first) == lane % PROPS)
        pick = jnp.where(pick, 1.0, 0.0).astype(jnp.bfloat16)
        fresh = jnp.dot(pick, fresh_all[:, 256:512], preferred_element_type=jnp.float32)
        at = lax.broadcasted_iota(jnp.int32, fresh.shape, 0) // HEADS - first
        inside = (at >= 0) & (at < PROPS)
        vo_ref[0] = jnp.where(inside, fresh, values.astype(jnp.float32)).astype(jnp.bfloat16)
        key_rows = SPAN * HEADS * 2
        lane = lax.broadcasted_iota(jnp.int32, (key_rows, HEADS * PROPS), 1)
        line = lax.broadcasted_iota(jnp.int32, (key_rows, HEADS * PROPS), 0)
        slot = lane // PROPS
        head = ((slot // 4 + zl) % 2) * 4 + (slot % 4 + y) % 4
        here = (((line // 2) % HEADS) == head) & ((line // 16 - first) == lane % PROPS)
        fresh = jnp.zeros((key_rows, HD), jnp.float32)
        for m in range(2):
            pick = jnp.where(here & (line % 2 == m), 1.0, 0.0).astype(jnp.bfloat16)
            fresh = fresh + jnp.dot(
                pick, fresh_all[:, m * HD : (m + 1) * HD], preferred_element_type=jnp.float32
            )
        at = lax.broadcasted_iota(jnp.int32, fresh.shape, 0) // 16 - first
        inside = (at >= 0) & (at < PROPS)
        ko_ref[0] = jnp.where(inside, fresh, keys.astype(jnp.float32)).astype(jnp.bfloat16)


def write_caches(scalars, keys, values, fresh):
    pairs = SPAN * HEADS
    key_spec = pl.BlockSpec((1, 2 * pairs, HD), lambda b, sc: (b, 0, 0))
    value_spec = pl.BlockSpec((1, pairs, 256), lambda b, sc: (b, 0, 0))
    new_spec = pl.BlockSpec(
        (1, PROPS, 512),
        lambda b, sc: (((b // SEQS - sc[0] + GROUPS) % GROUPS) * SEQS + b % SEQS, 0, 0),
    )
    return pl.pallas_call(
        write_kernel,
        grid_spec=pltpu.PrefetchScalarGridSpec(
            num_scalar_prefetch=1,
            grid=(GROUPS * SEQS,),
            in_specs=[key_spec, value_spec] + [new_spec] * HEADS,
            out_specs=[key_spec, value_spec],
        ),
        out_shape=[
            jax.ShapeDtypeStruct(keys.shape, jnp.bfloat16),
            jax.ShapeDtypeStruct(values.shape, jnp.bfloat16),
        ],
        cost_estimate=pl.CostEstimate(
            flops=2 * 10**9, transcendentals=0, bytes_accessed=10 * 2**20
        ),
        name="write_caches",
    )(scalars, keys, values, *fresh)


def visible_links(parents):
    number = parents.shape[-1]
    reached = jnp.eye(number, dtype=jnp.float32) + (
        parents[..., :, None] == jnp.arange(number, dtype=jnp.int32)
    ).astype(jnp.float32)
    for _ in range(4):
        reached = jnp.minimum(jnp.einsum("bij,bjk->bik", reached, reached), 1.0)
    depths = (jnp.sum(reached, axis=-1) - 1.0).astype(jnp.int32)
    return reached > 0.5, depths


def from_group(value, ahead):
    pairs = [((g + ahead) % GROUPS, g) for g in range(GROUPS)]
    return lax.ppermute(value, "zh", pairs)


def to_group(value, ahead):
    return lax.ppermute(value, "zh", [(g, (g + ahead) % GROUPS) for g in range(GROUPS)])


def fresh_rows(own):
    late = range(GROUPS // 2, GROUPS)
    stack = [own]
    for ahead in range(1, GROUPS):
        stack.append(lax.ppermute(own, "zh", [((g + ahead) % GROUPS, g) for g in late]))
    stack = jnp.concatenate(stack, axis=0)
    result = [stack]
    for slot in range(1, HEADS):
        pairs = []
        for g in late:
            for zl in range(2):
                for y in range(4):
                    source = ((zl + slot // 4) % 2) * 4 + (y + slot % 4) % 4
                    pairs.append((g * HEADS + source, g * HEADS + zl * 4 + y))
        result.append(lax.ppermute(stack, KV, pairs))
    return [r.reshape(GROUPS * SEQS, PROPS, 512) for r in result]


def rounded(x):
    return lax.reduce_precision(x, 8, 7)


def per_device(
    tokens,
    in_gain,
    query_weight,
    key_weight,
    value_weight,
    out_weight,
    lambdas,
    sub_gain,
    key_cache,
    value_cache,
    cache_len,
    accepted,
    parents,
):
    seq_count, prop_count, width_part = tokens.shape
    row_count = seq_count * prop_count
    zh = lax.axis_index("zh").astype(jnp.int32)
    zl = lax.axis_index("zl").astype(jnp.int32)
    y = lax.axis_index("y").astype(jnp.int32)
    head = zl * 4 + y
    starts = cache_len + accepted
    offset = (zh * HEADS + head) * SPAN
    pieces = packed_pieces(
        tokens.reshape(row_count, width_part),
        in_gain.reshape(1, width_part),
        query_weight,
        key_weight,
        value_weight,
    )
    arrived = lax.all_to_all(pieces, G, 0, 0, tiled=True)
    partial = projected(zh.reshape(1), arrived)
    shares = [partial[0]] + [to_group(partial[k], k) for k in range(1, GROUPS)]
    summed = shares[0].astype(jnp.float32)
    for share in shares[1:]:
        summed = summed + share.astype(jnp.float32)
    power = jnp.sum(summed[ROWS : ROWS + 3, 0:256], axis=0)
    power = lax.dynamic_slice(power, (zh * ROWS,), (ROWS,))
    row_scale = lax.rsqrt(power / D + 1e-06)
    scaled = summed[:ROWS] * row_scale[:, None]
    own_starts = lax.dynamic_slice(starts, (zh * SEQS,), (SEQS,))
    own_parents = lax.dynamic_slice(parents, (zh * SEQS, 0), (SEQS, prop_count))
    visible, depths = visible_links(own_parents)
    positions = (own_starts[:, None] + depths).reshape(ROWS)
    half_dim = HD // 2
    frequency = 10000.0 ** (-jnp.arange(half_dim, dtype=jnp.float32) / half_dim)
    angles = positions.astype(jnp.float32)[:, None] * frequency[None, :]
    cosine = jnp.cos(angles)[:, None]
    sine = jnp.sin(angles)[:, None]
    vectors = scaled[:, :512].reshape(ROWS, 4, HD)
    lower = vectors[..., :half_dim]
    upper = vectors[..., half_dim:]
    turned = jnp.concatenate(
        [lower * cosine - upper * sine, upper * cosine + lower * sine], axis=-1
    ).reshape(ROWS, 512)
    own_query = turned[:, :256].astype(jnp.bfloat16)
    own_new = jnp.concatenate([turned[:, 256:], scaled[:, 512:]], axis=1).astype(jnp.bfloat16)
    got = lax.all_to_all(
        jnp.broadcast_to(own_query[None], (GROUPS * HEADS, ROWS, 256)), KV, 0, 0, tiled=True
    ).reshape(GROUPS, HEADS, ROWS, 256)
    keys = key_cache.reshape(seq_count, SPAN * HEADS * 2, HD)
    values = value_cache.reshape(seq_count, SPAN * HEADS, 256)
    parts = attend(starts, offset.reshape(1), got, keys, values)
    columns = lax.all_to_all(out_weight.reshape(HEADS, 256, -1), G, 0, 0, tiled=True)
    fresh = fresh_rows(own_new)
    scalars = jnp.concatenate([jnp.stack([zh, zl, y, offset]), starts])
    key_out, value_out = write_caches(scalars, keys, values, fresh)

    met = lax.all_to_all(parts, G, 0, 0, tiled=True)
    levels = met[:, :, O_ROWS : O_ROWS + 3 * SEQS].astype(jnp.float32)
    levels = jnp.sum(
        levels.reshape(HEADS, GROUPS, SEQS, 3, 2, HEADS, PROPS), axis=3
    )
    levels = lax.dynamic_slice_in_dim(levels, head, 1, axis=4)[:, :, :, :, 0]
    top = jnp.max(levels, axis=0)
    share = jnp.exp(levels - top[None])
    total = jnp.sum(share, axis=0)
    share = share / total[None]
    level = top + jnp.log(total)
    merged = jnp.sum(
        met[:, :, :O_ROWS].astype(jnp.float32).reshape(HEADS, GROUPS, SEQS, 2, PROPS, 256)
        * share[..., None],
        axis=0,
    ).reshape(GROUPS, O_ROWS, 256)
    high = rounded(level)
    middle = rounded(level - high)
    low = rounded(level - high - middle)
    terms = jnp.stack([high, middle, low], axis=1).reshape(GROUPS, 3, O_ROWS)
    terms = jnp.pad(terms, ((0, 0), (0, 5), (0, 256 - O_ROWS)))
    bundle = jnp.concatenate([merged, terms], axis=1).astype(jnp.bfloat16)
    turn = [lax.dynamic_index_in_dim(bundle, (zh + k) % GROUPS, 0, False) for k in range(GROUPS)]
    sides = [turn[0]] + [to_group(turn[k], k) for k in range(1, GROUPS)]

    own_blocks = own_new.reshape(SEQS, PROPS, 4, HD)
    own_scores = jnp.einsum(
        "sqmd,sjmd->smqj",
        own_query.reshape(SEQS, PROPS, 2, HD),
        own_blocks[:, :, 0:2],
        preferred_element_type=jnp.float32,
    ) * (HD**-0.5)
    seen = visible[:, None]
    own_scores = jnp.where(seen, own_scores, NEG_FILL)
    levels = [
        jnp.sum(side[O_ROWS : O_ROWS + 3, :O_ROWS].astype(jnp.float32), axis=0).reshape(
            SEQS, 2, PROPS
        )
        for side in sides
    ]
    peak = jnp.max(own_scores, axis=-1)
    for level in levels:
        peak = jnp.maximum(peak, level)
    own_weight = jnp.where(seen, jnp.exp(own_scores - peak[..., None]), 0.0)
    total = jnp.sum(own_weight, axis=-1)
    portions = [jnp.exp(level - peak) for level in levels]
    for portion in portions:
        total = total + portion
    lam = lax.dynamic_slice(lambdas, (head,), (1,))
    sign = jnp.concatenate([jnp.ones((1,), jnp.float32), -lam])[None, :, None] / total
    own_weight = own_weight * sign[..., None]
    own_mix = jnp.sum(own_weight, axis=1).astype(jnp.bfloat16)
    own_values = own_new[:, 256:].reshape(SEQS, PROPS, 256)
    attended = jnp.einsum(
        "sqj,sje->sqe", own_mix, own_values, preferred_element_type=jnp.float32
    )
    for side, portion in zip(sides, portions):
        attended = attended + jnp.sum(
            side[:O_ROWS].astype(jnp.float32).reshape(SEQS, 2, PROPS, 256)
            * (portion * sign)[..., None],
            axis=1,
        )
    mixed = attended * lax.rsqrt(jnp.mean(attended * attended, axis=-1, keepdims=True) + 1e-05)
    mixed = (mixed * sub_gain.astype(jnp.float32) * LAMBDA_SCALE).astype(jnp.bfloat16)
    mixed = mixed.reshape(ROWS, 256)
    lines = [mixed] + [from_group(mixed, k) for k in range(1, GROUPS)]
    lines = jnp.stack(lines + lines[:-1])
    lines = lax.dynamic_slice_in_dim(lines, (GROUPS - zh) % GROUPS, GROUPS, axis=0)
    product = jnp.einsum(
        "re,pec->prc", lines.reshape(row_count, 256), columns, preferred_element_type=jnp.float32
    ).astype(jnp.bfloat16)
    halves = product.reshape(HEADS, row_count, 2, -1).transpose(0, 2, 1, 3)
    halves = halves.reshape(2 * HEADS, row_count, -1)
    met_out = lax.all_to_all(halves, ("zl", "y", "tp"), 0, 0, tiled=True)
    output = jnp.sum(met_out.astype(jnp.float32), axis=0).astype(jnp.bfloat16)
    output = output.reshape(seq_count, prop_count, -1)
    return (output, key_out.reshape(key_cache.shape), value_out.reshape(value_cache.shape))


def solution(mesh):
    torus = Mesh(
        mesh.devices.reshape(mesh.shape["dp"], GROUPS, 2, 4, mesh.shape["tp"]),
        ("dp", "zh", "zl", "y", "tp"),
    )
    placed = (
        P("dp", None, KV),
        P(KV),
        P(KV, "tp"),
        P(KV, "tp"),
        P(KV, "tp"),
        P("tp", KV),
        P("tp"),
        P(),
        P("dp", KV, "tp", None, None),
        P("dp", KV, "tp", None),
        P("dp"),
        P("dp"),
        P("dp", None),
    )
    return jax.shard_map(
        per_device,
        mesh=torus,
        in_specs=placed,
        out_specs=(
            P("dp", None, (*KV, "tp")),
            P("dp", KV, "tp", None, None),
            P("dp", KV, "tp", None),
        ),
        check_vma=False,
    )
```
